32 devices in a mesh: grp: 2 (over y), sp: 4 (over z), tp: 4 (over x, core).
Axes of the slice: x: 2, y: 2, z: 4, core: 2. Of those that a mesh axis runs over, the one named last changes fastest.
Arguments:
- conv_value: bfloat16 [4096, 1024], P(('grp', 'sp'), 'tp'), parts along dimension 0, may hold values from -6 to 6
- conv_gate: bfloat16 [4096, 1024], P(('grp', 'sp'), 'tp'), parts along dimension 0, may hold values from -6 to 6
- kernel: bfloat16 [31, 1024], P(None, 'tp'), may hold values from -4 to 4
- conv_bias: float32 [1024], P('tp'), may hold values from -3 to 3
- ln_gain: float32 [1024], P('tp'), may hold values from 0.1 to 1.9
- ln_bias: float32 [1024], P('tp'), may hold values from -3 to 3
- out_gain: float32 [1024], P('tp'), may hold values from 0.1 to 1.9
- out_weight: bfloat16 [1024, 2048], replicated, may hold values from -0.1875 to 0.1875
- residual: bfloat16 [4096, 2048], P(('grp', 'sp', 'tp')), parts along dimension 0, may hold values from -6 to 6
- moe_gain: float32 [2048], replicated, may hold values from 0.1 to 1.9
- expert_ids: int32 [4096, 2], P(('grp', 'sp', 'tp')), parts along dimension 0, may hold values from 0 to 15, as said below
- expert_weights: float32 [4096, 2], P(('grp', 'sp', 'tp')), parts along dimension 0, may hold values from 0.1 to 0.7
- w_gate: bfloat16 [16, 2048, 512], P(('sp', 'tp')), may hold values from -0.125 to 0.125
- w_up: bfloat16 [16, 2048, 512], P(('sp', 'tp')), may hold values from -0.125 to 0.125
- w_down: bfloat16 [16, 512, 2048], P(('sp', 'tp')), may hold values from -0.25 to 0.25
Outputs:
- layer_out: bfloat16 [4096, 2048], P(('grp', 'sp', 'tp')), parts along dimension 0
The draws below stay inside these ranges and needn't reach their ends.
There are 2 independent parts, one for each index of `grp`. The reference program is written for one: setup_inputs(seed, part) draws one part's arguments, and reference() takes and returns one part's arrays. A program takes and returns all parts, laid end to end along the dimension named above; an argument that names none is the same for every part. Nothing has to cross between parts.
Inputs may be any that keep to these rules, and one draw needn't show every extreme that they name: `expert_ids`: each row names two different experts of one group (group = expert number // 4). Among the 128 rows of one device (aligned blocks of 128 rows) no expert is named more than 32 times, and in every such block some expert is named exactly 32 times.
All inputs are finite; a program needn't handle non-finite values.
Results may differ from the reference program's by a relative error of at most 0.0095.
Values may be sent and summed in bfloat16 or wider, within the bound.
No kernel may reach another device: no remote copies, remote signals or barrier semaphores. Data moves between devices by JAX's collectives and lax.ppermute only.
A program may use at most 64 MiB of HBM per device.

```python
import jax
import jax.numpy as jnp
from jax import lax

D = 2048
CONV_CH = 1024
KERNEL = 31
HID = 512
ROWS = 128
TOKENS = 2048
EXPERTS = 16
EPG = 4
CAP = 32


def draw_kernel(key, part):
    key_base, key_jitter = jax.random.split(jax.random.fold_in(key, 11))
    ramp = jnp.exp(jnp.log(0.3) + jnp.log(10.0) * jnp.arange(CONV_CH, dtype=jnp.float32) / CONV_CH)
    jitter = jnp.exp(jax.random.uniform(key_jitter, (CONV_CH,), jnp.float32, -0.35, 0.35))
    base = jnp.clip(jax.random.normal(key_base, (KERNEL, CONV_CH), jnp.float32), -4.0, 4.0)
    return (base * ramp * jitter / jnp.sqrt(jnp.float32(KERNEL))).astype(jnp.bfloat16)


def draw_expert_ids(key, part):
    group_size = min(ROWS, EXPERTS // 2)
    rounds = TOKENS // group_size
    busiest = jax.random.randint(jax.random.fold_in(key, 21), (), 0, EXPERTS)
    round_keys = jax.random.split(jax.random.fold_in(key, 22), rounds)
    numbers = jnp.arange(EXPERTS, dtype=jnp.int32)

    def one_round(round_key):
        key_shift, key_order, key_mix, key_swap = jax.random.split(round_key, 4)
        shift_by = jax.random.randint(key_shift, (), 1, EPG)
        pre_image = busiest // EPG * EPG + (busiest % EPG - shift_by) % EPG
        scores = jax.random.permutation(key_order, EXPERTS).astype(jnp.int32)
        forced = (numbers == busiest) | (numbers == pre_image)
        scores = jnp.where(forced, scores + EXPERTS, scores)
        _, chosen = lax.top_k(scores, group_size)
        chosen = jax.random.permutation(key_mix, chosen.astype(jnp.int32))
        second = chosen // EPG * EPG + (chosen % EPG + shift_by) % EPG
        swapped = jax.random.randint(key_swap, (group_size,), 0, 2)
        first_col = jnp.where(swapped == 1, second, chosen)
        second_col = jnp.where(swapped == 1, chosen, second)
        return jnp.stack([first_col, second_col], axis=1).astype(jnp.int32)
    return jax.vmap(one_round)(round_keys).reshape(TOKENS, 2).astype(jnp.int32)


def block_levels(own_key, extent, shards, low, largest):
    def one(dim, shards_of):
        steps = jax.random.uniform(jax.random.fold_in(jax.random.fold_in(own_key, 6), dim), (shards_of,), jnp.float32, low / len(shards), largest / len(shards))
        return jnp.repeat(jnp.exp(steps), extent[dim] // shards_of).reshape((-1,) + (1,) * (len(extent) - dim - 1))

    level = one(*shards[0])
    for cut in shards[1:]:
        level = level * one(*cut)
    return level


def noise(stream_key, extent, scale, bound, shards=(), kind=jnp.bfloat16):
    array = scale * jax.random.normal(stream_key, extent, jnp.float32)
    if shards:
        array = array * block_levels(stream_key, extent, shards, -0.22, 0.18)
    return jnp.clip(array, -bound, bound).astype(kind)


def setup_inputs(seed: int = 0, part: int = 0) -> dict:
    keys = jax.random.split(jax.random.key(seed), 16)
    own_keys = jax.random.split(jax.random.fold_in(keys[15], part), 16)
    conv_value = noise(own_keys[0], (TOKENS, CONV_CH), 1.0, 6.0, ((0, 4), (1, 4)))
    conv_gate = noise(own_keys[1], (TOKENS, CONV_CH), 1.0, 6.0, ((0, 4), (1, 4)))
    kernel = draw_kernel(jax.random.fold_in(keys[15], 71), part)
    conv_bias = noise(keys[3], (CONV_CH,), 0.5, 3.0, ((0, 4),), jnp.float32)
    ln_gain = jnp.clip(1.0 + 0.18 * jax.random.normal(keys[4], (CONV_CH,), jnp.float32), 0.1, 1.9)
    ln_bias = noise(keys[5], (CONV_CH,), 0.5, 3.0, ((0, 4),), jnp.float32)
    out_gain = jnp.clip(1.0 + 0.18 * jax.random.normal(keys[6], (CONV_CH,), jnp.float32), 0.1, 1.9)
    out_weight = noise(keys[7], (CONV_CH, D), CONV_CH ** -0.5, 0.1875)
    residual = noise(own_keys[8], (TOKENS, D), 1.0, 6.0, ((0, 16),))
    moe_gain = jnp.clip(1.0 + 0.18 * jax.random.normal(keys[9], (D,), jnp.float32), 0.1, 1.9)
    expert_ids = draw_expert_ids(jax.random.fold_in(jax.random.fold_in(keys[15], part), 71), part)
    expert_weights = jnp.clip(0.1 + 0.59999999 * jax.random.uniform(own_keys[11], (TOKENS, 2), jnp.float32) ** block_levels(own_keys[11], (TOKENS, 2), ((0, 16),), -0.2, 0.2), 0.1, 0.7)
    w_gate = noise(keys[12], (EXPERTS, D, HID), D ** -0.5, 0.125, ((0, 16),))
    w_up = noise(keys[13], (EXPERTS, D, HID), D ** -0.5, 0.125, ((0, 16),))
    w_down = noise(keys[14], (EXPERTS, HID, D), HID ** -0.5, 0.25, ((0, 16),))
    return dict(conv_value=conv_value, conv_gate=conv_gate, kernel=kernel, conv_bias=conv_bias, ln_gain=ln_gain, ln_bias=ln_bias, out_gain=out_gain, out_weight=out_weight, residual=residual, moe_gain=moe_gain, expert_ids=expert_ids, expert_weights=expert_weights, w_gate=w_gate, w_up=w_up, w_down=w_down)


EPSILON = 1e-06

def reference(conv_value, conv_gate, kernel, conv_bias, ln_gain, ln_bias, out_gain, out_weight, residual, moe_gain, expert_ids, expert_weights, w_gate, w_up, w_down):
    gated = (conv_value.astype(jnp.float32) * jax.nn.sigmoid(conv_gate.astype(jnp.float32))).astype(jnp.bfloat16)
    padded = jnp.concatenate([jnp.zeros((KERNEL - 1, CONV_CH), gated.dtype), gated], axis=0)
    convolved = jnp.zeros((TOKENS, CONV_CH), jnp.float32) + conv_bias
    for offset in range(KERNEL):
        convolved = convolved + padded[offset:offset + TOKENS].astype(jnp.float32) * kernel[offset].astype(jnp.float32)
    average = lax.optimization_barrier(jnp.mean(convolved, axis=1, keepdims=True))
    spread = lax.optimization_barrier(jnp.mean(convolved * convolved, axis=1, keepdims=True)) - average * average
    swished = jax.nn.silu((convolved - average) * lax.rsqrt(spread + EPSILON) * ln_gain + ln_bias)
    energy = lax.optimization_barrier(jnp.mean(swished * swished, axis=1, keepdims=True))
    branch = (swished * lax.rsqrt(energy + EPSILON) * out_gain).astype(jnp.bfloat16)
    projected = jnp.dot(branch, out_weight, preferred_element_type=jnp.float32)
    hidden = (residual.astype(jnp.float32) + projected).astype(jnp.bfloat16)
    widened = hidden.astype(jnp.float32)
    normed = (widened * lax.rsqrt(lax.optimization_barrier(jnp.mean(widened * widened, axis=1, keepdims=True)) + EPSILON) * moe_gain).astype(jnp.bfloat16)
    flat_ids = expert_ids.reshape(-1).astype(jnp.int32)
    onehot = (flat_ids[:, None] == jnp.arange(EXPERTS, dtype=jnp.int32)[None, :]).astype(jnp.int32)
    slot_rank = lax.optimization_barrier(jnp.sum((jnp.cumsum(onehot, axis=0) - 1) * onehot, axis=1)).astype(jnp.int32)
    capacity = TOKENS // ROWS * CAP
    position = flat_ids * capacity + slot_rank
    token_index = (jnp.arange(2 * TOKENS, dtype=jnp.int32) // 2).astype(jnp.int32)
    table = jnp.full((EXPERTS * capacity,), TOKENS, jnp.int32).at[position].set(token_index).reshape(EXPERTS, capacity)
    weight_table = jnp.zeros((EXPERTS * capacity,), jnp.float32).at[position].set(expert_weights.reshape(-1).astype(jnp.float32)).reshape(EXPERTS, capacity)
    source_rows = jnp.concatenate([normed, jnp.zeros((1, D), normed.dtype)], axis=0)

    def one_expert(total, pieces):
        rows_index, row_weights, gate_w, up_w, down_w = pieces
        taken = source_rows[rows_index]
        gate_part = jnp.dot(taken, gate_w, preferred_element_type=jnp.float32)
        up_part = jnp.dot(taken, up_w, preferred_element_type=jnp.float32)
        active = (jax.nn.silu(gate_part) * up_part).astype(jnp.bfloat16)
        result = jnp.dot(active, down_w, preferred_element_type=jnp.float32).astype(jnp.bfloat16)
        return (total.at[rows_index].add(row_weights[:, None] * result.astype(jnp.float32)), None)
    start_total = jnp.zeros((TOKENS + 1, D), jnp.float32)
    combined, _ = lax.scan(one_expert, start_total, (table, weight_table, w_gate, w_up, w_down))
    return (widened + combined[:TOKENS]).astype(jnp.bfloat16)
```

```python
import jax
import jax.numpy as jnp
from jax import lax
from jax.sharding import PartitionSpec as P

EPSILON = 1e-06
GROUPS = 4
CHOICES = 2
LANES = 128

F32 = jnp.float32
BF16 = jnp.bfloat16


def passed_along(block, axis, distance):
    devices = range(lax.axis_size(axis))
    route = [(i - distance, i) for i in devices if i - distance in devices]
    return lax.ppermute(block, axis, route)


def shifted(block, axis, distance):
    size = lax.axis_size(axis)
    if distance % size == 0:
        return block
    return lax.ppermute(block, axis, [(i, (i + distance) % size) for i in range(size)])


def halves(value):
    high = lax.reduce_precision(value, 8, 7)
    low = lax.reduce_precision(value - high, 8, 7)
    return high.astype(BF16), low.astype(BF16)


def ranks(hits):
    rows = hits.shape[0]
    earlier = lax.broadcasted_iota(jnp.int32, (rows, rows), 1) < lax.broadcasted_iota(
        jnp.int32, (rows, rows), 0
    )
    return jnp.dot(
        earlier.astype(BF16), hits.astype(BF16), preferred_element_type=F32
    ).astype(jnp.int32)


def placed(hits, slots):
    rank = ranks(hits)
    numbers = lax.broadcasted_iota(jnp.int32, hits.shape + (slots,), 2)
    return hits[:, :, None] & (rank[:, :, None] == numbers)


def packed(selection, rows):
    return lax.dot_general(
        selection, rows, (((0,), (0,)), ((), ())), preferred_element_type=F32
    ).astype(BF16)


def per_device(
    conv_value,
    conv_gate,
    kernel,
    conv_bias,
    ln_gain,
    ln_bias,
    out_gain,
    out_weight,
    residual,
    moe_gain,
    expert_ids,
    expert_weights,
    w_gate,
    w_up,
    w_down,
):
    n_sp = lax.axis_size("sp")
    n_tp = lax.axis_size("tp")
    my_sp = lax.axis_index("sp")
    my_tp = lax.axis_index("tp")
    tok_rows, channels = conv_value.shape
    reach_rows = kernel.shape[0] - 1
    full_channels = channels * n_tp
    row_count = tok_rows // n_tp
    width = residual.shape[1]
    experts = n_sp * n_tp
    capacity = CHOICES * row_count // min(row_count, experts // CHOICES)
    slots = capacity * n_tp
    if n_tp % (experts // GROUPS) == 0:
        slots = slots // CHOICES
    slots = min(slots, row_count)

    gated = (conv_value.astype(F32) * jax.nn.sigmoid(conv_gate.astype(F32))).astype(BF16)
    before = passed_along(gated[tok_rows - reach_rows :], "sp", 1)
    padded = jnp.concatenate([before, gated], axis=0)
    convolved = jnp.zeros((tok_rows, channels), F32) + conv_bias
    for offset in range(reach_rows + 1):
        convolved = convolved + padded[offset : offset + tok_rows].astype(F32) * kernel[
            offset
        ].astype(F32)
    convolved = convolved.astype(BF16).reshape(n_tp, row_count, channels)

    gain_rows = [half for gain in (ln_gain, ln_bias, out_gain) for half in halves(gain)]
    gain_block = jnp.concatenate(
        [jnp.stack(gain_rows), jnp.zeros((16 - len(gain_rows), channels), BF16)], axis=0
    )
    regrouped = jnp.zeros((row_count + 16, full_channels), BF16)
    for k in range(n_tp):
        piece = lax.dynamic_index_in_dim(convolved, (my_tp + k) % n_tp, 0, keepdims=False)
        piece = shifted(jnp.concatenate([piece, gain_block], axis=0), "tp", k)
        regrouped = lax.dynamic_update_slice(
            regrouped, piece, (0, (my_tp - k) % n_tp * channels)
        )
    gains = regrouped[row_count:].astype(F32)
    full_ln_gain = (gains[0] + gains[1])[None]
    full_ln_bias = (gains[2] + gains[3])[None]
    full_out_gain = (gains[4] + gains[5])[None]
    conv = regrouped[:row_count].astype(F32)
    average = jnp.mean(conv, axis=1, keepdims=True)
    spread = jnp.mean(conv * conv, axis=1, keepdims=True) - average * average
    swished = jax.nn.silu((conv - average) * lax.rsqrt(spread + EPSILON) * full_ln_gain + full_ln_bias)
    energy = jnp.mean(swished * swished, axis=1, keepdims=True)
    branch = (swished * lax.rsqrt(energy + EPSILON) * full_out_gain).astype(BF16)
    projected = jnp.dot(branch, out_weight, preferred_element_type=F32)
    hidden = (residual.astype(F32) + projected).astype(BF16)
    widened = hidden.astype(F32)
    normed = (
        widened * lax.rsqrt(jnp.mean(widened * widened, axis=1, keepdims=True) + EPSILON) * moe_gain
    ).astype(BF16)

    columns = (my_sp + jnp.arange(n_sp, dtype=jnp.int32)) % n_sp
    homes = expert_ids // n_tp
    going = (homes[:, 0:1] == columns[None]) | (homes[:, 1:2] == columns[None])
    outward = placed(going, slots).astype(BF16)
    weight_high, weight_low = halves(expert_weights)
    notes = jnp.concatenate(
        [
            (expert_ids + 1).astype(BF16),
            weight_high,
            weight_low,
            jnp.zeros((row_count, LANES - 3 * CHOICES), BF16),
        ],
        axis=1,
    )
    noted = jnp.concatenate([normed, notes], axis=1)

    order = [0] + sorted(range(1, n_sp), key=lambda k: -min(k, n_sp - k))
    per_chunk = -(-n_sp // GROUPS)
    chunks = [order[i : i + per_chunk] for i in range(0, n_sp, per_chunk)]
    arrived = {}
    for k in order:
        arrived[k] = shifted(packed(outward[:, k], noted), "sp", k)

    locals_ = (my_tp + jnp.arange(n_tp, dtype=jnp.int32)) % n_tp
    inward = {}

    def one_chunk(members):
        boxes = []
        for k in members:
            marks = arrived[k][:, width : width + 3 * CHOICES].astype(F32)
            named = marks[:, :CHOICES].astype(jnp.int32) - 1 - my_sp * n_tp
            weights = marks[:, CHOICES : 2 * CHOICES] + marks[:, 2 * CHOICES :]
            hits = [named[:, i : i + 1] == locals_[None] for i in range(CHOICES)]
            place = placed(hits[0] | hits[1], capacity)
            inward[k] = [
                (
                    (place & hit[:, :, None]).astype(BF16).reshape(slots, n_tp * capacity),
                    weights[:, i : i + 1],
                )
                for i, hit in enumerate(hits)
            ]
            select = place.astype(BF16).reshape(slots, n_tp * capacity)
            boxes.append(packed(select, arrived[k][:, :width]).reshape(n_tp, capacity, width))
        sent = []
        for m in range(n_tp):
            box = jnp.concatenate([b[m] for b in boxes], axis=0)
            sent.append(shifted(box, "tp", m))
        rows = jnp.concatenate(sent, axis=0)
        gate_part = jnp.dot(rows, w_gate[0], preferred_element_type=F32)
        up_part = jnp.dot(rows, w_up[0], preferred_element_type=F32)
        active = (jax.nn.silu(gate_part) * up_part).astype(BF16)
        result = jnp.dot(active, w_down[0], preferred_element_type=F32).astype(BF16)
        result = result.reshape(n_tp, len(members), capacity, width)
        back = [shifted(result[m], "tp", -m) for m in range(n_tp)]
        sums = {}
        for i, k in enumerate(members):
            mine = jnp.concatenate([b[i] for b in back], axis=0)
            total = 0.0
            for select, weight in inward[k]:
                total = total + weight * jnp.dot(select, mine, preferred_element_type=F32)
            sums[k] = shifted(total.astype(BF16), "sp", -k)
        return sums

    combined = widened
    for members in chunks:
        for k, block in one_chunk(members).items():
            combined = combined + jnp.dot(outward[:, k], block, preferred_element_type=F32)
    return combined.astype(BF16)


def solution(mesh):
    in_specs = (
        P(("grp", "sp"), "tp"),
        P(("grp", "sp"), "tp"),
        P(None, "tp"),
        P("tp"),
        P("tp"),
        P("tp"),
        P("tp"),
        P(),
        P(("grp", "sp", "tp"), None),
        P(),
        P(("grp", "sp", "tp"), None),
        P(("grp", "sp", "tp"), None),
        P(("sp", "tp"), None, None),
        P(("sp", "tp"), None, None),
        P(("sp", "tp"), None, None),
    )
    out_specs = P(("grp", "sp", "tp"), None)
    return jax.shard_map(
        per_device, mesh=mesh, in_specs=in_specs, out_specs=out_specs, check_vma=False
    )
```

```python
import functools

import jax
import jax.numpy as jnp
from jax import lax
from jax.sharding import PartitionSpec as P


EPSILON = 1e-06
GROUPS = 4
CHOICES = 2
LANES = 128
FAR_FIRST = 1
CHUNKS = [[0], [1], [2], [3]]
BATCHES = [[0], [1], [2], [3]]

F32 = jnp.float32
BF16 = jnp.bfloat16


def passed_along(block, axis, distance):
    devices = range(lax.axis_size(axis))
    route = [(i - distance, i) for i in devices if i - distance in devices]
    return lax.ppermute(block, axis, route)


def shifted(block, axis, distance):
    size = lax.axis_size(axis)
    if distance % size == 0:
        return block
    return lax.ppermute(block, axis, [(i, (i + distance) % size) for i in range(size)])


def halves(value):
    high = lax.reduce_precision(value, 8, 7)
    low = lax.reduce_precision(value - high, 8, 7)
    return high.astype(BF16), low.astype(BF16)


def ranks(hits):
    rows = hits.shape[0]
    earlier = lax.broadcasted_iota(jnp.int32, (rows, rows), 1) < lax.broadcasted_iota(
        jnp.int32, (rows, rows), 0
    )
    return jnp.dot(
        earlier.astype(BF16), hits.astype(BF16), preferred_element_type=F32
    ).astype(jnp.int32)


def placed(hits, numbers):
    return hits & (ranks(hits) == numbers)


def packed(selection, rows):
    return lax.dot_general(
        selection, rows, (((0,), (0,)), ((), ())), preferred_element_type=F32
    ).astype(BF16)


def per_device(
    conv_value,
    conv_gate,
    kernel,
    conv_bias,
    ln_gain,
    ln_bias,
    out_gain,
    out_weight,
    residual,
    moe_gain,
    expert_ids,
    expert_weights,
    w_gate,
    w_up,
    w_down,
):
    n_sp = lax.axis_size("sp")
    n_tp = lax.axis_size("tp")
    my_sp = lax.axis_index("sp")
    my_tp = lax.axis_index("tp")
    tok_rows, channels = conv_value.shape
    reach_rows = kernel.shape[0] - 1
    full_channels = channels * n_tp
    row_count = tok_rows // n_tp
    width = residual.shape[1]
    experts = n_sp * n_tp
    capacity = CHOICES * row_count // min(row_count, experts // CHOICES)
    slots = capacity * n_tp
    if n_tp % (experts // GROUPS) == 0:
        slots = slots // CHOICES
    slots = min(slots, row_count)

    gated = (conv_value.astype(F32) * jax.nn.sigmoid(conv_gate.astype(F32))).astype(BF16)
    before = passed_along(gated[tok_rows - reach_rows :], "sp", 1)
    padded = jnp.concatenate([before, gated], axis=0)
    convolved = jnp.zeros((tok_rows, channels), F32) + conv_bias
    for offset in range(reach_rows + 1):
        convolved = convolved + padded[offset : offset + tok_rows].astype(F32) * kernel[
            offset
        ].astype(F32)
    convolved = convolved.astype(BF16).reshape(n_tp, row_count, channels)

    gain_rows = [half for gain in (ln_gain, ln_bias, out_gain) for half in halves(gain)]
    gain_block = jnp.concatenate(
        [jnp.stack(gain_rows), jnp.zeros((16 - len(gain_rows), channels), BF16)], axis=0
    )
    regrouped = jnp.zeros((row_count + 16, full_channels), BF16)
    for k in range(n_tp):
        piece = lax.dynamic_index_in_dim(convolved, (my_tp + k) % n_tp, 0, keepdims=False)
        piece = shifted(jnp.concatenate([piece, gain_block], axis=0), "tp", k)
        regrouped = lax.dynamic_update_slice(
            regrouped, piece, (0, (my_tp - k) % n_tp * channels)
        )
    gains = regrouped[row_count:].astype(F32)
    full_ln_gain = (gains[0] + gains[1])[None]
    full_ln_bias = (gains[2] + gains[3])[None]
    full_out_gain = (gains[4] + gains[5])[None]
    conv = regrouped[:row_count].astype(F32)
    average = jnp.mean(conv, axis=1, keepdims=True)
    spread = jnp.mean(conv * conv, axis=1, keepdims=True) - average * average
    swished = jax.nn.silu((conv - average) * lax.rsqrt(spread + EPSILON) * full_ln_gain + full_ln_bias)
    energy = jnp.mean(swished * swished, axis=1, keepdims=True)
    branch = (swished * lax.rsqrt(energy + EPSILON) * full_out_gain).astype(BF16)
    projected = jnp.dot(branch, out_weight, preferred_element_type=F32)
    hidden = (residual.astype(F32) + projected).astype(BF16)
    widened = hidden.astype(F32)
    normed = (
        widened * lax.rsqrt(jnp.mean(widened * widened, axis=1, keepdims=True) + EPSILON) * moe_gain
    ).astype(BF16)

    column = lax.broadcasted_iota(jnp.int32, (row_count, n_sp * slots), 1)
    target = (my_sp + column // slots) % n_sp
    homes = expert_ids // n_tp
    going = functools.reduce(
        jnp.logical_or, [homes[:, i : i + 1] == target for i in range(CHOICES)]
    )
    spots = placed(going, column % slots).astype(BF16)
    outward = {k: spots[:, k * slots : (k + 1) * slots] for k in range(n_sp)}
    weight_high, weight_low = halves(expert_weights)
    notes = jnp.concatenate(
        [
            (expert_ids + 1).astype(BF16),
            weight_high,
            weight_low,
            jnp.zeros((row_count, LANES - 3 * CHOICES), BF16),
        ],
        axis=1,
    )
    noted = jnp.concatenate([normed, notes], axis=1)

    order = [0] + sorted(range(1, n_sp), key=lambda k: FAR_FIRST * min(k, n_sp - k))
    per_chunk = -(-n_sp // GROUPS)
    blocks = [order[i : i + per_chunk] for i in range(0, n_sp, per_chunk)]
    chunks = [sum((blocks[i] for i in chunk if i < len(blocks)), []) for chunk in CHUNKS]
    chunks = [chunk for chunk in chunks if chunk]
    batches = [sum((chunks[c] for c in batch if c < len(chunks)), []) for batch in BATCHES]
    batches = [batch for batch in batches if batch]
    arrived = {}
    for members in chunks:
        for k in members:
            block = packed(outward[k], noted)
            arrived[k] = shifted(block, "sp", k)

    inward = {}
    boxes = {}
    previous = None
    for members in chunks:
        pieces = [[] for _ in range(n_tp)]
        for k in members:
            block = arrived[k]
            if previous is not None:
                block, _ = lax.optimization_barrier((block, previous))
            marks = block[:, width : width + 3 * CHOICES].astype(F32)
            named = marks[:, :CHOICES].astype(jnp.int32) - 1 - my_sp * n_tp
            weights = marks[:, CHOICES : 2 * CHOICES] + marks[:, 2 * CHOICES :]
            column = lax.broadcasted_iota(jnp.int32, (slots, n_tp * capacity), 1)
            local = (my_tp + column // capacity) % n_tp
            hits = [named[:, i : i + 1] == local for i in range(CHOICES)]
            place = placed(functools.reduce(jnp.logical_or, hits), column % capacity)
            share = sum(jnp.where(hit, weights[:, i : i + 1], 0.0) for i, hit in enumerate(hits))
            inward[k] = jnp.where(place, share, 0.0).astype(BF16)
            select = place.astype(BF16)
            for m in range(n_tp):
                pieces[m].append(
                    packed(select[:, m * capacity : (m + 1) * capacity], block[:, :width])
                )
            previous = pieces[-1][-1]
        for m in range(n_tp):
            for k, piece in zip(members, pieces[m]):
                boxes[k, m] = piece
            if m:
                whole = shifted(jnp.concatenate(pieces[m], axis=0), "tp", m)
                for i, k in enumerate(members):
                    boxes[k, m] = whole[i * capacity : (i + 1) * capacity]

    sums = {}
    for members in batches:
        rows = jnp.concatenate(
            [boxes[k, m] for m in range(n_tp) for k in members], axis=0
        )
        gate_part = jnp.dot(rows, w_gate[0], preferred_element_type=F32)
        up_part = jnp.dot(rows, w_up[0], preferred_element_type=F32)
        active = (jax.nn.silu(gate_part) * up_part).astype(BF16)
        result = jnp.dot(active, w_down[0], preferred_element_type=F32).astype(BF16)
        result = result.reshape(n_tp, len(members) * capacity, width)
        back = [shifted(result[m], "tp", -m) for m in range(n_tp)]
        for i, k in enumerate(members):
            mine = jnp.concatenate(
                [p[i * capacity : (i + 1) * capacity] for p in back], axis=0
            )
            total = jnp.dot(inward[k], mine, preferred_element_type=F32).astype(BF16)
            sums[k] = shifted(total, "sp", -k)

    early = [k for members in batches[:-1] for k in members]
    late = batches[-1]
    combined = widened
    for part in (early, late):
        if part:
            combined = combined + jnp.dot(
                jnp.concatenate([outward[k] for k in part], axis=1),
                jnp.concatenate([sums[k] for k in part], axis=0),
                preferred_element_type=F32,
            )
    return combined.astype(BF16)


def solution(mesh):
    in_specs = (
        P(("grp", "sp"), "tp"),
        P(("grp", "sp"), "tp"),
        P(None, "tp"),
        P("tp"),
        P("tp"),
        P("tp"),
        P("tp"),
        P(),
        P(("grp", "sp", "tp"), None),
        P(),
        P(("grp", "sp", "tp"), None),
        P(("grp", "sp", "tp"), None),
        P(("sp", "tp"), None, None),
        P(("sp", "tp"), None, None),
        P(("sp", "tp"), None, None),
    )
    out_specs = P(("grp", "sp", "tp"), None)

    return jax.shard_map(
        per_device, mesh=mesh, in_specs=in_specs, out_specs=out_specs, check_vma=False
    )
```
